32 devices in a mesh: sp: 16 (over z, y, x), tp: 2 (over core).
Axes of the slice: x: 2, y: 2, z: 4, core: 2. Of those that a mesh axis runs over, the one named last changes fastest.
Arguments:
- mid_rows: bfloat16 [4096, 2048], P(('sp', 'tp')), may hold values from -6 to 6
- cotangent: bfloat16 [4096, 2048], P(('sp', 'tp')), may hold values from -6 to 6
- routes: int32 [4096, 2], P(('sp', 'tp')), may hold values from 0 to 15, all different within a row; in each aligned block of 128 rows (0 to 127, 128 to 255, ...) at most 32 rows name the same one
- route_weight: float32 [4096, 2], P(('sp', 'tp')), may hold values from 0.3 to 2
- filtered: bfloat16 [4096, 2048], P('sp', 'tp'), may hold values from -30 to 30
- conv_taps: float32 [31, 2048], P(None, 'tp'), may hold values from -1 to 1
- norm_gain: float32 [2048], P('tp'), may hold values from 0.1 to 1.9
- out_weight: bfloat16 [2048, 2048], P('tp'), may hold values from -0.125 to 0.125
- gate_weight: bfloat16 [16, 2048, 1024], P('sp', None, 'tp'), may hold values from -0.125 to 0.125
- up_weight: bfloat16 [16, 2048, 1024], P('sp', None, 'tp'), may hold values from -0.125 to 0.125
- down_weight: bfloat16 [16, 1024, 2048], P('sp', 'tp'), may hold values from -0.1875 to 0.1875
Outputs:
- gate_grad: float32 [16, 2048, 1024], P('sp', None, 'tp')
- up_grad: float32 [16, 2048, 1024], P('sp', None, 'tp')
- down_grad: float32 [16, 1024, 2048], P('sp', 'tp')
- proj_grad: float32 [2048, 2048], P('sp', 'tp')
- input_grad: bfloat16 [4096, 2048], P('sp', 'tp')
The draws below stay inside these ranges and needn't reach their ends.
Inputs may be any that keep to these rules, and one draw needn't show every extreme that they name: `routes`: each row names 2 different experts. In each aligned block of 128 rows no expert is named by more than 32 rows.
All inputs are finite; a program needn't handle non-finite values.
Results may differ from the reference program's by a relative error of at most 0.0075.
Values may be sent and summed in bfloat16 or wider, within the bound.
A program may use at most 128 MiB of HBM per device.

```python
import math
import jax
import jax.numpy as jnp
import numpy as np
from jax import lax

D = 2048
FFE = 1024
TAPS = 31
TOPK = 2
EXPERTS = 16
TOKENS = 4096
ROWS_DEV = 128
CAP = 32
N_SP = 16
N_TP = 2


def draw_filtered(key, part):
    base_key, chan_key, row_key = jax.random.split(key, 3)
    channel = jnp.arange(D)
    block_factor = jnp.where(channel >= D // 2, 3.0, 1.0)
    spread = jnp.exp(jax.random.uniform(chan_key, (D,), jnp.float32, -0.7, 0.7))
    values = jnp.clip(jax.random.normal(base_key, (TOKENS, D), jnp.float32), -4.0, 4.0)
    return (values * block_factor * spread).astype(jnp.bfloat16)


def raised(values, own_key, source, target, shards_of, factor):
    def block_of(dim):
        return (jnp.arange(values.shape[dim]) // (values.shape[dim] // shards_of)).reshape((-1,) + (1,) * (values.ndim - 1 - dim))

    one_side = jax.random.permutation(own_key, shards_of)[block_of(target)]
    second = (block_of(target) + shards_of // 2) % shards_of
    return jnp.where((block_of(source) == one_side) | (block_of(source) == second), factor * values, values)


def block_levels(own_key, extent, cuts, smallest, top_value):
    gain, own = 1.0, jax.random.fold_in(own_key, 6)
    for axis_at, blocks in cuts:
        steps = jnp.exp(jax.random.uniform(jax.random.fold_in(own, axis_at), (blocks,), jnp.float32, smallest / len(cuts), top_value / len(cuts)))
        gain = gain * jnp.repeat(steps, extent[axis_at] // blocks).reshape([-1 if axis == axis_at else 1 for axis in range(len(extent))])
    return gain


def deal_out(stream_key, own, number, rows, count, top, limit, lean):
    sequence = jax.random.permutation(stream_key, count)
    heavy_load, common = portions_of(count, rows * top, limit, lean, True), portions_of(count, rows * top, limit, lean, False)
    places = jnp.arange(count)

    def named(lengths, offset_by):
        used = int((lengths > 0).sum())
        fixed = max(1, used // 4)
        moved = fixed + (places - fixed + offset_by * (used - fixed)) % max(1, count - fixed)
        return jnp.zeros((count,), jnp.int32).at[sequence[jnp.where(places < fixed, places, moved)]].set(jnp.asarray(lengths, jnp.int32))

    lengths = jnp.where(number % 4 == 0, named(heavy_load, number // 4), named(common, number - number // 4 - 1))
    mixed = jax.random.permutation(jax.random.fold_in(own, 3), count)
    source_of, taker = mixed[0:count // 2 * 2:2], mixed[1:count // 2 * 2:2]
    slack = jnp.minimum(lengths[source_of] - 1, limit - lengths[taker]) // 2
    slack = jnp.where((source_of == sequence[0]) | (taker == sequence[0]) | (lengths[taker] == 0), 0, jnp.maximum(slack, 0))
    moved = jax.random.randint(jax.random.fold_in(own, 4), (count // 2,), 0, 1 << 20) % (slack + 1)
    lengths = lengths.at[source_of].add(-moved).at[taker].add(moved)
    labels = jnp.searchsorted(jnp.cumsum(lengths), jnp.arange(rows * top), side="right").astype(jnp.int32)
    grid = labels.reshape(top, rows).T
    grid = grid[jax.random.permutation(jax.random.fold_in(own, 1), rows)]
    offset_by = jax.random.randint(jax.random.fold_in(own, 2), (rows, 1), 0, top)
    return jnp.take_along_axis(grid, (jnp.arange(top)[None, :] + offset_by) % top, axis=1)


def portions_of(number_of, total, bound, skew, full):
    weights = [(1 << 20) // math.isqrt(rank ** skew) + 1 for rank in range(1, number_of + 1)]
    largest = bound if full else min(bound, max(-(-total // number_of), total * weights[0] // sum(weights)))
    least = 1 if total - largest >= number_of - 1 else 0
    holding, rest = [largest] + [least] * (number_of - 1), total - largest - least * (number_of - 1)
    while rest > 0:
        candidates = [i for i in range(1, number_of) if holding[i] < largest] or [i for i in range(1, number_of) if holding[i] < bound]
        pool, budget = sum([weights[i] for i in candidates]), rest
        for i in candidates:
            addition = min(bound - holding[i], max(1, budget * weights[i] // pool), rest)
            holding[i] = holding[i] + addition
            rest = rest - addition
    return np.array(holding)


def gaussian(rng, shape, scale, limit, cuts=(), kind=jnp.bfloat16):
    level = block_levels(rng, shape, cuts, -0.22, 0.18) if cuts else 1.0
    values = jax.random.normal(rng, shape, jnp.float32) * scale * level
    return jnp.minimum(jnp.maximum(values, -limit), limit).astype(kind)


def bell_draw_with(key, dims, deviation, bound, cuts, heavy, kind=jnp.bfloat16):
    values = deviation * jax.random.normal(key, dims, jnp.float32)
    if cuts:
        values = values * block_levels(key, dims, cuts, -0.22, 0.18)
    return jnp.clip(raised(values, jax.random.fold_in(key, 3), *heavy), -bound, bound).astype(kind)


def setup_inputs(seed: int = 0) -> dict:
    keys = jax.random.split(jax.random.key(seed), 12)
    mid_rows = gaussian(keys[0], (TOKENS, D), 1.0, 6.0, ((0, 32),))
    cotangent = bell_draw_with(keys[1], (TOKENS, D), 1.0, 6.0, ((0, 32),), (0, 1, 32, 2.75))
    routes_keys = jax.random.split(jax.random.fold_in(keys[2], 1), TOKENS // ROWS_DEV)
    routes_turns = jax.random.permutation(jax.random.fold_in(keys[2], 3), TOKENS // ROWS_DEV)
    routes = jax.vmap(lambda own, number: deal_out(jax.random.fold_in(keys[2], 2), own, number, ROWS_DEV, EXPERTS, TOPK, CAP, 2))(routes_keys, routes_turns).reshape((TOKENS, TOPK))
    route_weight = jnp.clip(jnp.exp(math.log(2.0) - 1.89712 * jax.random.uniform(keys[3], (TOKENS, TOPK), jnp.float32) ** block_levels(keys[3], (TOKENS, TOPK), ((0, 32),), -0.2, 0.2)), 0.3, 2.0)
    filtered = draw_filtered(jax.random.fold_in(keys[11], 71), 0)
    conv_taps = gaussian(keys[5], (TAPS, D), TAPS ** -0.5, 1.0, ((1, 2),), jnp.float32)
    norm_gain = jnp.clip(1.0 + 0.18 * jax.random.normal(keys[6], (D,), jnp.float32), 0.1, 1.9)
    out_weight = gaussian(keys[7], (D, D), D ** -0.5, 0.125, ((0, 2),))
    gate_weight = gaussian(keys[8], (EXPERTS, D, FFE), D ** -0.5, 0.125, ((0, 16), (2, 2)))
    up_weight = gaussian(keys[9], (EXPERTS, D, FFE), D ** -0.5, 0.125, ((0, 16), (2, 2)))
    down_weight = gaussian(keys[10], (EXPERTS, FFE, D), FFE ** -0.5, 0.1875, ((0, 16), (1, 2)))
    return dict(mid_rows=mid_rows, cotangent=cotangent, routes=routes, route_weight=route_weight, filtered=filtered, conv_taps=conv_taps, norm_gain=norm_gain, out_weight=out_weight, gate_weight=gate_weight, up_weight=up_weight, down_weight=down_weight)


NORM_EPS = 1e-05

def silu_grad(pre_act):
    logistic = jax.nn.sigmoid(pre_act)
    return logistic * (1.0 + pre_act * (1.0 - logistic))

def reference(mid_rows, cotangent, routes, route_weight, filtered, conv_taps, norm_gain, out_weight, gate_weight, up_weight, down_weight):
    total_routes = TOKENS * TOPK
    flattened = routes.reshape(total_routes)
    weight_flat = jnp.concatenate([route_weight.reshape(total_routes), jnp.zeros((1,), jnp.float32)])
    route_ids = jnp.arange(total_routes, dtype=jnp.int32)
    slot_total = N_SP * N_TP * CAP
    half_width = FFE // N_TP

    def expert_step(collected, expert):
        chosen = flattened == expert
        positions = jnp.cumsum(chosen.astype(jnp.int32)) - 1
        target = jnp.where(chosen, positions, slot_total).astype(jnp.int32)
        slot_owner = jnp.full((slot_total + 1,), total_routes, jnp.int32).at[target].set(route_ids)[:slot_total]
        token_of = (slot_owner // TOPK).astype(jnp.int32)
        inputs = jnp.take(mid_rows, token_of, axis=0, mode='fill', fill_value=0)
        cot_rows = jnp.take(cotangent, token_of, axis=0, mode='fill', fill_value=0).astype(jnp.float32)
        route_scale = weight_flat[slot_owner]
        routed = (route_scale[:, None] * cot_rows).astype(jnp.bfloat16)
        gate_mat = gate_weight[expert]
        up_mat = up_weight[expert]
        down_mat = down_weight[expert]
        pre_gate = jnp.dot(inputs, gate_mat, preferred_element_type=jnp.float32)
        pre_up = jnp.dot(inputs, up_mat, preferred_element_type=jnp.float32)
        gate_act = jax.nn.silu(pre_gate)
        hidden = (gate_act * pre_up).astype(jnp.bfloat16)
        down_part = jnp.dot(hidden.T, routed, preferred_element_type=jnp.float32)
        hidden_grad = jnp.dot(routed, down_mat.T, preferred_element_type=jnp.float32)
        gate_pre = (hidden_grad * pre_up * silu_grad(pre_gate)).astype(jnp.bfloat16)
        up_pre = (hidden_grad * gate_act).astype(jnp.bfloat16)
        gate_part = jnp.dot(inputs.T, gate_pre, preferred_element_type=jnp.float32)
        up_part = jnp.dot(inputs.T, up_pre, preferred_element_type=jnp.float32)
        summed = jnp.zeros((slot_total, D), jnp.float32)
        for band_index in range(N_TP):
            band_start = band_index * half_width
            band_stop = band_start + half_width
            band_term = jnp.dot(gate_pre[:, band_start:band_stop], gate_mat[:, band_start:band_stop].T, preferred_element_type=jnp.float32)
            band_term = band_term + jnp.dot(up_pre[:, band_start:band_stop], up_mat[:, band_start:band_stop].T, preferred_element_type=jnp.float32)
            summed = summed + lax.optimization_barrier(band_term.astype(jnp.bfloat16)).astype(jnp.float32)
        route_grad = summed.astype(jnp.bfloat16)
        collected = collected.at[slot_owner].set(route_grad)
        return (collected, (gate_part, up_part, down_part))
    start_rows = jnp.zeros((total_routes + 1, D), jnp.bfloat16)
    collected, (gate_grad, up_grad, down_grad) = lax.scan(expert_step, start_rows, jnp.arange(EXPERTS, dtype=jnp.int32))
    route_sum = lax.optimization_barrier(jnp.sum(collected[:total_routes].astype(jnp.float32).reshape(TOKENS, TOPK, D), axis=1))
    mid_grad = (cotangent.astype(jnp.float32) + route_sum).astype(jnp.bfloat16)
    values = filtered.astype(jnp.float32)
    average = lax.optimization_barrier(jnp.mean(values, axis=1, keepdims=True))
    variance = lax.optimization_barrier(jnp.mean(values * values, axis=1, keepdims=True)) - average * average
    inv_scale = lax.rsqrt(variance + NORM_EPS)
    normed = (values - average) * inv_scale
    scaled = normed * norm_gain
    activated = jax.nn.silu(scaled).astype(jnp.bfloat16)
    proj_grad = jnp.dot(mid_grad.T, activated, preferred_element_type=jnp.float32)
    act_grad = jnp.dot(mid_grad, out_weight.T, preferred_element_type=jnp.float32)
    scaled_grad = act_grad * silu_grad(scaled) * norm_gain
    grad_mean = lax.optimization_barrier(jnp.mean(scaled_grad, axis=1, keepdims=True))
    grad_corr = lax.optimization_barrier(jnp.mean(scaled_grad * normed, axis=1, keepdims=True))
    conv_grad = (inv_scale * (scaled_grad - grad_mean - normed * grad_corr)).astype(jnp.bfloat16)
    halo_width = TAPS // 2
    padded = jnp.pad(conv_grad, ((halo_width, halo_width), (0, 0))).astype(jnp.float32)
    accumulated = jnp.zeros((TOKENS, D), jnp.float32)
    for offset in range(TAPS):
        lead = 2 * halo_width - offset
        accumulated = accumulated + conv_taps[offset] * padded[lead:lead + TOKENS]
    input_grad = accumulated.astype(jnp.bfloat16)
    return (gate_grad, up_grad, down_grad, proj_grad, input_grad)
```

```python
import jax
import jax.numpy as jnp
from jax import lax
from jax.sharding import PartitionSpec as P

NORM_EPS = 1e-05


def extended(block, sides, width):
    for axis, dim in sides:
        count = lax.axis_size(axis)
        forward = [(i, i + 1) for i in range(count - 1)]
        backward = [(target, source) for source, target in forward]
        low = lax.ppermute(
            lax.slice_in_dim(block, block.shape[dim] - width, None, axis=dim), axis, forward
        )
        high = lax.ppermute(lax.slice_in_dim(block, 0, width, axis=dim), axis, backward)
        block = jnp.concatenate([low, block, high], axis=dim)
    return block


def silu_grad(pre_act):
    logistic = jax.nn.sigmoid(pre_act)
    return logistic * (1.0 + pre_act * (1.0 - logistic))


def slot_targets(routes, experts, capacity):
    token_count, per_token = routes.shape
    flattened = routes.reshape(token_count * per_token)
    one_hot = flattened[:, None] == jnp.arange(experts, dtype=jnp.int32)[None, :]
    route_ids = jnp.arange(token_count * per_token, dtype=jnp.int32)
    before = (route_ids[None, :] < route_ids[:, None]).astype(jnp.bfloat16)
    earlier = jnp.dot(before, one_hot.astype(jnp.bfloat16), preferred_element_type=jnp.float32)
    positions = jnp.sum(jnp.where(one_hot, earlier, 0.0), axis=1).astype(jnp.int32)
    return (flattened * capacity + positions).reshape(token_count, per_token)


def halving_orders(count):
    bits = count.bit_length() - 1
    turned = min(bits, 3)
    return [
        [(start + step) % turned for step in range(turned)] + list(range(turned, bits))
        for start in range(turned)
    ]


def column_groups(columns, groups):
    lanes = 128
    tiles = columns // lanes
    sizes = [tiles // groups + (1 if g < tiles % groups else 0) for g in range(groups)]
    starts = [sum(sizes[:g]) * lanes for g in range(groups)]
    return [(start, size * lanes) for start, size in zip(starts, sizes) if size]


def picked(block, place, dim):
    return lax.dynamic_index_in_dim(block, place, dim, keepdims=False)


def token_product(rows, columns):
    flat = rows.reshape(rows.shape[0], -1)
    return lax.dot_general(
        flat, columns, (((0,), (0,)), ((), ())), preferred_element_type=jnp.float32
    ).reshape(rows.shape[1:] + (columns.shape[1],))


def reduced_products(rows, columns, axis):
    count = lax.axis_size(axis)
    tokens, width = rows.shape
    bits = count.bit_length() - 1
    own = lax.axis_index(axis)
    cut = rows.reshape((tokens,) + (2,) * bits + (width // count,))
    orders = halving_orders(count)
    pieces = []
    for order, (start, size) in zip(orders, column_groups(columns.shape[1], len(orders))):
        group = lax.slice_in_dim(columns, start, start + size, axis=1)
        left = list(range(bits - 1, -1, -1))
        total = None
        for bit in order:
            mine = (own >> bit) & 1
            dim = left.index(bit)
            if total is None:
                outgoing = token_product(picked(cut, 1 - mine, dim + 1), group)
                kept = token_product(picked(cut, mine, dim + 1), group)
            else:
                outgoing = picked(total, 1 - mine, dim)
                kept = picked(total, mine, dim)
            pairs = [(i, i ^ (1 << bit)) for i in range(count)]
            arrived = lax.ppermute(outgoing.astype(jnp.bfloat16), axis, pairs)
            total = kept + arrived.astype(jnp.float32)
            left.pop(dim)
        pieces.append(total)
    return jnp.concatenate(pieces, axis=1)


def expert_backward(inputs, routed, gate_mat, up_mat, down_mat):
    pre_gate = jnp.einsum("secd,edf->secf", inputs, gate_mat, preferred_element_type=jnp.float32)
    pre_up = jnp.einsum("secd,edf->secf", inputs, up_mat, preferred_element_type=jnp.float32)
    gate_act = jax.nn.silu(pre_gate)
    hidden = (gate_act * pre_up).astype(jnp.bfloat16)
    down_part = jnp.einsum("secf,secd->efd", hidden, routed, preferred_element_type=jnp.float32)
    hidden_grad = jnp.einsum("secd,efd->secf", routed, down_mat, preferred_element_type=jnp.float32)
    gate_pre = (hidden_grad * pre_up * silu_grad(pre_gate)).astype(jnp.bfloat16)
    up_pre = (hidden_grad * gate_act).astype(jnp.bfloat16)
    gate_part = jnp.einsum("secd,secf->edf", inputs, gate_pre, preferred_element_type=jnp.float32)
    up_part = jnp.einsum("secd,secf->edf", inputs, up_pre, preferred_element_type=jnp.float32)
    return (gate_pre, up_pre, gate_part, up_part, down_part)


def input_part(gate_pre, up_pre, gate_mat, up_mat):
    first_term = jnp.einsum(
        "secf,edf->secd", gate_pre, gate_mat, preferred_element_type=jnp.float32
    )
    return first_term + jnp.einsum(
        "secf,edf->secd", up_pre, up_mat, preferred_element_type=jnp.float32
    )


def per_device(
    mid_rows,
    cotangent,
    routes,
    route_weight,
    filtered,
    conv_taps,
    norm_gain,
    out_weight,
    gate_weight,
    up_weight,
    down_weight,
):
    sp_count = lax.axis_size("sp")
    token_count, model_width = mid_rows.shape
    per_token = routes.shape[1]
    local_experts = gate_weight.shape[0]
    experts = local_experts * sp_count
    capacity = 2 * token_count * per_token // sp_count
    values = filtered.astype(jnp.float32)
    channel_sum, squares = lax.psum(
        (jnp.sum(values, axis=1), jnp.sum(values * values, axis=1)), "tp"
    )
    target = slot_targets(routes, experts, capacity)
    slot_ids = jnp.arange(experts * capacity, dtype=jnp.int32)
    holds = slot_ids[:, None, None] == target[None, :, :]
    chosen = jnp.any(holds, axis=2).astype(jnp.bfloat16)
    route_scale = jnp.sum(jnp.where(holds, route_weight[None, :, :], 0.0), axis=(1, 2))
    inputs = jnp.dot(chosen, mid_rows, preferred_element_type=jnp.float32).astype(jnp.bfloat16)
    cot_rows = jnp.dot(chosen, cotangent, preferred_element_type=jnp.float32)
    routed = (route_scale[:, None] * cot_rows).astype(jnp.bfloat16)
    inputs = inputs.reshape(sp_count, local_experts, capacity, model_width)
    routed = routed.reshape(sp_count, local_experts, capacity, model_width)
    got_in = lax.all_to_all(inputs, "sp", split_axis=0, concat_axis=0, tiled=True)
    got_cot = lax.all_to_all(routed, "sp", split_axis=0, concat_axis=0, tiled=True)
    all_in = lax.all_gather(got_in, "tp", axis=0, tiled=True)
    all_cot = lax.all_gather(got_cot, "tp", axis=0, tiled=True)
    gate_pre, up_pre, gate_part, up_part, down_part = expert_backward(
        all_in, all_cot, gate_weight, up_weight, down_weight
    )
    partial_rows = input_part(gate_pre, up_pre, gate_weight, up_weight).astype(jnp.bfloat16)
    back_rows = (
        lax.psum_scatter(partial_rows, "tp", scatter_dimension=0, tiled=True)
        .astype(jnp.float32)
        .astype(jnp.bfloat16)
    )
    returned = lax.all_to_all(back_rows, "sp", split_axis=0, concat_axis=0, tiled=True)
    gate_grad, up_grad, down_grad = (gate_part, up_part, down_part)
    back_all = returned.reshape(experts * capacity, model_width)
    route_sum = lax.dot_general(
        chosen, back_all, (((0,), (0,)), ((), ())), preferred_element_type=jnp.float32
    )
    mid_grad = (cotangent.astype(jnp.float32) + route_sum).astype(jnp.bfloat16)
    average = channel_sum / model_width
    variance = squares / model_width - average * average
    inv_scale = lax.rsqrt(variance + NORM_EPS)[:, None]
    normed = (values - average[:, None]) * inv_scale
    scaled = normed * norm_gain
    activated = jax.nn.silu(scaled).astype(jnp.bfloat16)
    grad_tokens = lax.all_gather(mid_grad, "tp", axis=0, tiled=True)
    proj_grad = reduced_products(grad_tokens, activated, "sp")
    act_grad = lax.dot_general(
        grad_tokens, out_weight, (((1,), (1,)), ((), ())), preferred_element_type=jnp.float32
    )
    scaled_grad = act_grad * silu_grad(scaled) * norm_gain
    grad_total, corr_total = lax.psum(
        (jnp.sum(scaled_grad, axis=1), jnp.sum(scaled_grad * normed, axis=1)), "tp"
    )
    grad_mean = (grad_total / model_width)[:, None]
    grad_corr = (corr_total / model_width)[:, None]
    conv_grad = (inv_scale * (scaled_grad - grad_mean - normed * grad_corr)).astype(jnp.bfloat16)
    halo_width = conv_taps.shape[0] // 2
    padded = extended(conv_grad, (("sp", 0),), halo_width)
    seq_rows = conv_grad.shape[0]
    accumulated = jnp.zeros(conv_grad.shape, jnp.float32)
    for offset in range(conv_taps.shape[0]):
        lead = 2 * halo_width - offset
        accumulated = accumulated + conv_taps[offset] * padded[lead : lead + seq_rows]
    input_grad = accumulated.astype(jnp.bfloat16)
    return (gate_grad, up_grad, down_grad, proj_grad, input_grad)


def solution(mesh):
    in_specs = (
        P(("sp", "tp"), None),
        P(("sp", "tp"), None),
        P(("sp", "tp"), None),
        P(("sp", "tp"), None),
        P("sp", "tp"),
        P(None, "tp"),
        P("tp"),
        P("tp", None),
        P("sp", None, "tp"),
        P("sp", None, "tp"),
        P("sp", "tp", None),
    )
    out_specs = (
        P("sp", None, "tp"),
        P("sp", None, "tp"),
        P("sp", "tp", None),
        P("sp", "tp"),
        P("sp", "tp"),
    )
    return jax.shard_map(
        per_device, mesh=mesh, in_specs=in_specs, out_specs=out_specs, check_vma=False
    )
```

```python
import jax
import jax.numpy as jnp
from jax import lax
from jax.sharding import PartitionSpec as P

NORM_EPS = 1e-05


def extended(block, sides, width):
    for axis, dim in sides:
        count = lax.axis_size(axis)
        forward = [(i, i + 1) for i in range(count - 1)]
        backward = [(target, source) for source, target in forward]
        low = lax.ppermute(
            lax.slice_in_dim(block, block.shape[dim] - width, None, axis=dim), axis, forward
        )
        high = lax.ppermute(lax.slice_in_dim(block, 0, width, axis=dim), axis, backward)
        block = jnp.concatenate([low, block, high], axis=dim)
    return block


def silu_grad(pre_act):
    logistic = jax.nn.sigmoid(pre_act)
    return logistic * (1.0 + pre_act * (1.0 - logistic))


def slot_targets(routes, experts, capacity):
    token_count, per_token = routes.shape
    flattened = routes.reshape(token_count * per_token)
    one_hot = flattened[:, None] == jnp.arange(experts, dtype=jnp.int32)[None, :]
    route_ids = jnp.arange(token_count * per_token, dtype=jnp.int32)
    before = (route_ids[None, :] < route_ids[:, None]).astype(jnp.bfloat16)
    earlier = jnp.dot(before, one_hot.astype(jnp.bfloat16), preferred_element_type=jnp.float32)
    positions = jnp.sum(jnp.where(one_hot, earlier, 0.0), axis=1).astype(jnp.int32)
    return (flattened * capacity + positions).reshape(token_count, per_token)


def halving_orders(count):
    bits = count.bit_length() - 1
    turned = min(bits, 3)
    return [
        [(start + step) % turned for step in range(turned)] + list(range(turned, bits))
        for start in range(turned)
    ]


def column_groups(columns, groups):
    lanes = 128
    tiles = columns // lanes
    sizes = [tiles // groups + (1 if g < tiles % groups else 0) for g in range(groups)]
    starts = [sum(sizes[:g]) * lanes for g in range(groups)]
    return [(start, size * lanes) for start, size in zip(starts, sizes) if size]


def picked(block, place, dim):
    return lax.dynamic_index_in_dim(block, place, dim, keepdims=False)


def reduced_products(rows, columns, axis):
    count = lax.axis_size(axis)
    tokens, width = rows.shape
    bits = count.bit_length() - 1
    own = lax.axis_index(axis)
    product = transposed_product(rows, columns).astype(jnp.bfloat16)
    cut = product.reshape((2,) * bits + (width // count, columns.shape[1]))
    orders = halving_orders(count)
    pieces = []
    for order, (start, size) in zip(orders, column_groups(columns.shape[1], len(orders))):
        total = lax.slice_in_dim(cut, start, start + size, axis=bits + 1)
        left = list(range(bits - 1, -1, -1))
        for bit in order:
            mine = (own >> bit) & 1
            dim = left.index(bit)
            outgoing = picked(total, 1 - mine, dim)
            kept = picked(total, mine, dim).astype(jnp.float32)
            pairs = [(i, i ^ (1 << bit)) for i in range(count)]
            arrived = lax.ppermute(outgoing.astype(jnp.bfloat16), axis, pairs)
            total = kept + arrived.astype(jnp.float32)
            left.pop(dim)
        pieces.append(total)
    return jnp.concatenate(pieces, axis=1)


def row_product(rows, matrix, dim=0):
    return lax.dot_general(
        rows, matrix, (((1,), (dim,)), ((), ())), preferred_element_type=jnp.float32
    )


def transposed_product(left, right):
    return lax.dot_general(
        left, right, (((0,), (0,)), ((), ())), preferred_element_type=jnp.float32
    )


def from_partner(block, axis):
    count = lax.axis_size(axis)
    return [
        lax.ppermute(block, axis, [(i, (i + step) % count) for i in range(count)])
        for step in range(1, count)
    ]


def hidden_gradients(pre_gate, pre_up, routed, down_mat):
    gate_act = jax.nn.silu(pre_gate)
    hidden = (gate_act * pre_up).astype(jnp.bfloat16)
    hidden_grad = row_product(routed, down_mat, 1)
    gate_pre = (hidden_grad * pre_up * silu_grad(pre_gate)).astype(jnp.bfloat16)
    up_pre = (hidden_grad * gate_act).astype(jnp.bfloat16)
    return hidden, gate_pre, up_pre


def input_part(gate_pre, up_pre, gate_mat, up_mat):
    return (row_product(gate_pre, gate_mat, 1) + row_product(up_pre, up_mat, 1)).astype(
        jnp.bfloat16
    )


def expert_backward(got_in, got_cot, gate_mat, up_mat, down_mat, axis):
    count = lax.axis_size(axis)
    all_in = [got_in] + from_partner(got_in, axis)
    pre = [(row_product(rows, gate_mat), row_product(rows, up_mat)) for rows in all_in]
    all_cot = [got_cot] + from_partner(got_cot, axis)
    grads = [hidden_gradients(g, u, c, down_mat) for (g, u), c in zip(pre, all_cot)]
    back = None
    for step in range(1, count):
        part = input_part(grads[step][1], grads[step][2], gate_mat, up_mat)
        arrived = lax.ppermute(part, axis, [(i, (i - step) % count) for i in range(count)])
        back = (arrived,) if back is None else back + (arrived,)
    back_rows = input_part(grads[0][1], grads[0][2], gate_mat, up_mat).astype(jnp.float32)
    for arrived in back or ():
        back_rows = back_rows + arrived.astype(jnp.float32)
    gate_part = sum(transposed_product(x, g[1]) for x, g in zip(all_in, grads))
    up_part = sum(transposed_product(x, g[2]) for x, g in zip(all_in, grads))
    down_part = sum(transposed_product(g[0], c) for g, c in zip(grads, all_cot))
    return gate_part, up_part, down_part, back_rows.astype(jnp.bfloat16)


def gathered_rows(block, axis):
    count = lax.axis_size(axis)
    own = lax.axis_index(axis)
    blocks = [block] + from_partner(block, axis)
    turned = jnp.concatenate(blocks, axis=0)
    result = turned
    for place in range(1, count):
        order = [blocks[(place - i) % count] for i in range(count)]
        result = jnp.where(own == place, jnp.concatenate(order, axis=0), result)
    first = [blocks[-i % count] for i in range(count)]
    return jnp.where(own == 0, jnp.concatenate(first, axis=0), result)


def per_device(
    mid_rows,
    cotangent,
    routes,
    route_weight,
    filtered,
    conv_taps,
    norm_gain,
    out_weight,
    gate_weight,
    up_weight,
    down_weight,
):
    sp_count = lax.axis_size("sp")
    token_count, model_width = mid_rows.shape
    per_token = routes.shape[1]
    local_experts = gate_weight.shape[0]
    experts = local_experts * sp_count
    capacity = 2 * token_count * per_token // sp_count
    values = filtered.astype(jnp.float32)
    channel_sum, squares = lax.psum(
        (jnp.sum(values, axis=1), jnp.sum(values * values, axis=1)), "tp"
    )
    target = slot_targets(routes, experts, capacity)
    slot_ids = jnp.arange(experts * capacity, dtype=jnp.int32)
    holds = slot_ids[:, None, None] == target[None, :, :]
    chosen = jnp.any(holds, axis=2).astype(jnp.bfloat16)
    route_scale = jnp.sum(jnp.where(holds, route_weight[None, :, :], 0.0), axis=(1, 2))
    inputs = jnp.dot(chosen, mid_rows, preferred_element_type=jnp.float32).astype(jnp.bfloat16)
    cot_rows = jnp.dot(chosen, cotangent, preferred_element_type=jnp.float32)
    routed = (route_scale[:, None] * cot_rows).astype(jnp.bfloat16)
    inputs = inputs.reshape(sp_count, local_experts, capacity, model_width)
    routed = routed.reshape(sp_count, local_experts, capacity, model_width)
    got_in = lax.all_to_all(inputs, "sp", split_axis=0, concat_axis=0, tiled=True)
    got_cot = lax.all_to_all(routed, "sp", split_axis=0, concat_axis=0, tiled=True)
    by_expert = (sp_count, local_experts, capacity, model_width)
    parts = [
        expert_backward(
            got_in[:, e].reshape(sp_count * capacity, model_width),
            got_cot[:, e].reshape(sp_count * capacity, model_width),
            gate_weight[e],
            up_weight[e],
            down_weight[e],
            "tp",
        )
        for e in range(local_experts)
    ]
    gate_grad, up_grad, down_grad = (
        jnp.stack([part[i] for part in parts], axis=0) for i in range(3)
    )
    back_rows = jnp.stack(
        [part[3].reshape(sp_count, capacity, model_width) for part in parts], axis=1
    ).reshape(by_expert)
    returned = lax.all_to_all(back_rows, "sp", split_axis=0, concat_axis=0, tiled=True)
    back_all = returned.reshape(experts * capacity, model_width)
    route_sum = lax.dot_general(
        chosen, back_all, (((0,), (0,)), ((), ())), preferred_element_type=jnp.float32
    )
    mid_grad = (cotangent.astype(jnp.float32) + route_sum).astype(jnp.bfloat16)
    average = channel_sum / model_width
    variance = squares / model_width - average * average
    inv_scale = lax.rsqrt(variance + NORM_EPS)[:, None]
    normed = (values - average[:, None]) * inv_scale
    scaled = normed * norm_gain
    activated = jax.nn.silu(scaled).astype(jnp.bfloat16)
    grad_tokens = gathered_rows(mid_grad, "tp")
    proj_grad = reduced_products(grad_tokens, activated, "sp")
    act_grad = lax.dot_general(
        grad_tokens, out_weight, (((1,), (1,)), ((), ())), preferred_element_type=jnp.float32
    )
    scaled_grad = act_grad * silu_grad(scaled) * norm_gain
    grad_total, corr_total = lax.psum(
        (jnp.sum(scaled_grad, axis=1), jnp.sum(scaled_grad * normed, axis=1)), "tp"
    )
    grad_mean = (grad_total / model_width)[:, None]
    grad_corr = (corr_total / model_width)[:, None]
    conv_grad = (inv_scale * (scaled_grad - grad_mean - normed * grad_corr)).astype(jnp.bfloat16)
    halo_width = conv_taps.shape[0] // 2
    padded = extended(conv_grad, (("sp", 0),), halo_width)
    seq_rows = conv_grad.shape[0]
    accumulated = jnp.zeros(conv_grad.shape, jnp.float32)
    for offset in range(conv_taps.shape[0]):
        lead = 2 * halo_width - offset
        accumulated = accumulated + conv_taps[offset] * padded[lead : lead + seq_rows]
    input_grad = accumulated.astype(jnp.bfloat16)
    return (gate_grad, up_grad, down_grad, proj_grad, input_grad)


def solution(mesh):
    in_specs = (
        P(("sp", "tp"), None),
        P(("sp", "tp"), None),
        P(("sp", "tp"), None),
        P(("sp", "tp"), None),
        P("sp", "tp"),
        P(None, "tp"),
        P("tp"),
        P("tp", None),
        P("sp", None, "tp"),
        P("sp", None, "tp"),
        P("sp", "tp", None),
    )
    out_specs = (
        P("sp", None, "tp"),
        P("sp", None, "tp"),
        P("sp", "tp", None),
        P("sp", "tp"),
        P("sp", "tp"),
    )
    return jax.shard_map(
        per_device, mesh=mesh, in_specs=in_specs, out_specs=out_specs, check_vma=False
    )
```

```python
import jax
import jax.numpy as jnp
from jax import lax
from jax.sharding import PartitionSpec as P

NORM_EPS = 1e-05


def extended(block, sides, width):
    for axis, dim in sides:
        count = lax.axis_size(axis)
        forward = [(i, i + 1) for i in range(count - 1)]
        backward = [(target, source) for source, target in forward]
        low = lax.ppermute(
            lax.slice_in_dim(block, block.shape[dim] - width, None, axis=dim), axis, forward
        )
        high = lax.ppermute(lax.slice_in_dim(block, 0, width, axis=dim), axis, backward)
        block = jnp.concatenate([low, block, high], axis=dim)
    return block


def silu_grad(pre_act):
    logistic = jax.nn.sigmoid(pre_act)
    return logistic * (1.0 + pre_act * (1.0 - logistic))


def slot_targets(routes, experts, capacity):
    token_count, per_token = routes.shape
    flattened = routes.reshape(token_count * per_token)
    one_hot = flattened[:, None] == jnp.arange(experts, dtype=jnp.int32)[None, :]
    route_ids = jnp.arange(token_count * per_token, dtype=jnp.int32)
    before = (route_ids[None, :] < route_ids[:, None]).astype(jnp.bfloat16)
    earlier = jnp.dot(before, one_hot.astype(jnp.bfloat16), preferred_element_type=jnp.float32)
    positions = jnp.sum(jnp.where(one_hot, earlier, 0.0), axis=1).astype(jnp.int32)
    return (flattened * capacity + positions).reshape(token_count, per_token)


def halving_orders(count):
    bits = count.bit_length() - 1
    turned = min(bits, 3)
    return [
        [(start + step) % turned for step in range(turned)] + list(range(turned, bits))
        for start in range(turned)
    ]


def column_groups(columns, groups):
    lanes = 128
    tiles = columns // lanes
    sizes = [tiles // groups + (1 if g < tiles % groups else 0) for g in range(groups)]
    starts = [sum(sizes[:g]) * lanes for g in range(groups)]
    return [(start, size * lanes) for start, size in zip(starts, sizes) if size]


def picked(block, place, dim):
    return lax.dynamic_index_in_dim(block, place, dim, keepdims=False)


def reduced_products(rows, columns, axis):
    count = lax.axis_size(axis)
    tokens, width = rows.shape
    bits = count.bit_length() - 1
    own = lax.axis_index(axis)
    product = transposed_product(rows, columns).astype(jnp.bfloat16)
    cut = product.reshape((2,) * bits + (width // count, columns.shape[1]))
    orders = halving_orders(count)
    groups = column_groups(columns.shape[1], len(orders))
    orders = orders[: len(groups)]
    totals = [lax.slice_in_dim(cut, start, start + size, axis=bits + 1) for start, size in groups]
    left = [list(range(bits - 1, -1, -1)) for _ in groups]
    for step in range(bits):
        outgoing, kept = [], []
        for total, order, dims in zip(totals, orders, left):
            mine = (own >> order[step]) & 1
            dim = dims.index(order[step])
            dims.pop(dim)
            outgoing.append(picked(total, 1 - mine, dim).astype(jnp.bfloat16))
            kept.append(picked(total, mine, dim).astype(jnp.float32))
        if step == 0:
            outgoing, rows = lax.optimization_barrier((outgoing, rows))
        arrived = [
            lax.ppermute(block, axis, [(i, i ^ (1 << order[step])) for i in range(count)])
            for block, order in zip(outgoing, orders)
        ]
        arrived = lax.optimization_barrier(arrived)
        totals = [own_part + got.astype(jnp.float32) for own_part, got in zip(kept, arrived)]
    return jnp.concatenate(totals, axis=1), rows


def row_product(rows, matrix, dim=0):
    return lax.dot_general(
        rows, matrix, (((1,), (dim,)), ((), ())), preferred_element_type=jnp.float32
    )


def transposed_product(left, right):
    return lax.dot_general(
        left, right, (((0,), (0,)), ((), ())), preferred_element_type=jnp.float32
    )


def from_partner(block, axis):
    count = lax.axis_size(axis)
    return [
        lax.ppermute(block, axis, [(i, (i + step) % count) for i in range(count)])
        for step in range(1, count)
    ]


def hidden_gradients(pre_gate, pre_up, routed, down_mat):
    gate_act = jax.nn.silu(pre_gate)
    hidden = (gate_act * pre_up).astype(jnp.bfloat16)
    hidden_grad = row_product(routed, down_mat, 1)
    gate_pre = (hidden_grad * pre_up * silu_grad(pre_gate)).astype(jnp.bfloat16)
    up_pre = (hidden_grad * gate_act).astype(jnp.bfloat16)
    return hidden, gate_pre, up_pre


def input_part(gate_pre, up_pre, gate_mat, up_mat):
    return (row_product(gate_pre, gate_mat, 1) + row_product(up_pre, up_mat, 1)).astype(
        jnp.bfloat16
    )


def expert_backward(got_in, got_cot, gate_mat, up_mat, down_mat, axis):
    count = lax.axis_size(axis)
    all_in = [got_in] + from_partner(got_in, axis)
    pre = [(row_product(rows, gate_mat), row_product(rows, up_mat)) for rows in all_in]
    pre, got_cot = lax.optimization_barrier((pre, got_cot))
    all_cot = [got_cot] + from_partner(got_cot, axis)
    grads = [hidden_gradients(g, u, c, down_mat) for (g, u), c in zip(pre, all_cot)]
    back = None
    for step in range(1, count):
        part = input_part(grads[step][1], grads[step][2], gate_mat, up_mat)
        arrived = lax.ppermute(part, axis, [(i, (i - step) % count) for i in range(count)])
        back = (arrived,) if back is None else back + (arrived,)
    back_rows = input_part(grads[0][1], grads[0][2], gate_mat, up_mat).astype(jnp.float32)
    for arrived in back or ():
        back_rows = back_rows + arrived.astype(jnp.float32)
    gate_part = sum(transposed_product(x, g[1]) for x, g in zip(all_in, grads))
    up_part = sum(transposed_product(x, g[2]) for x, g in zip(all_in, grads))
    down_part = sum(transposed_product(g[0], c) for g, c in zip(grads, all_cot))
    return gate_part, up_part, down_part, back_rows.astype(jnp.bfloat16)


def gathered_rows(block, axis):
    count = lax.axis_size(axis)
    own = lax.axis_index(axis)
    blocks = [block] + from_partner(block, axis)
    turned = jnp.concatenate(blocks, axis=0)
    result = turned
    for place in range(1, count):
        order = [blocks[(place - i) % count] for i in range(count)]
        result = jnp.where(own == place, jnp.concatenate(order, axis=0), result)
    first = [blocks[-i % count] for i in range(count)]
    return jnp.where(own == 0, jnp.concatenate(first, axis=0), result)


def per_device(
    mid_rows,
    cotangent,
    routes,
    route_weight,
    filtered,
    conv_taps,
    norm_gain,
    out_weight,
    gate_weight,
    up_weight,
    down_weight,
):
    sp_count = lax.axis_size("sp")
    token_count, model_width = mid_rows.shape
    per_token = routes.shape[1]
    local_experts = gate_weight.shape[0]
    experts = local_experts * sp_count
    capacity = 2 * token_count * per_token // sp_count
    values = filtered.astype(jnp.float32)
    channel_sum, squares = lax.psum(
        (jnp.sum(values, axis=1), jnp.sum(values * values, axis=1)), "tp"
    )
    target = slot_targets(routes, experts, capacity)
    slot_ids = jnp.arange(experts * capacity, dtype=jnp.int32)
    holds = slot_ids[:, None, None] == target[None, :, :]
    chosen = jnp.any(holds, axis=2).astype(jnp.bfloat16)
    route_scale = jnp.sum(jnp.where(holds, route_weight[None, :, :], 0.0), axis=(1, 2))
    inputs = jnp.dot(chosen, mid_rows, preferred_element_type=jnp.float32).astype(jnp.bfloat16)
    cot_rows = jnp.dot(chosen, cotangent, preferred_element_type=jnp.float32)
    routed = (route_scale[:, None] * cot_rows).astype(jnp.bfloat16)
    inputs = inputs.reshape(sp_count, local_experts, capacity, model_width)
    routed = routed.reshape(sp_count, local_experts, capacity, model_width)
    got_in = lax.all_to_all(inputs, "sp", split_axis=0, concat_axis=0, tiled=True)
    got_cot = lax.all_to_all(routed, "sp", split_axis=0, concat_axis=0, tiled=True)
    by_expert = (sp_count, local_experts, capacity, model_width)
    parts = [
        expert_backward(
            got_in[:, e].reshape(sp_count * capacity, model_width),
            got_cot[:, e].reshape(sp_count * capacity, model_width),
            gate_weight[e],
            up_weight[e],
            down_weight[e],
            "tp",
        )
        for e in range(local_experts)
    ]
    gate_grad, up_grad, down_grad = (
        jnp.stack([part[i] for part in parts], axis=0) for i in range(3)
    )
    back_rows = jnp.stack(
        [part[3].reshape(sp_count, capacity, model_width) for part in parts], axis=1
    ).reshape(by_expert)
    returned = lax.all_to_all(back_rows, "sp", split_axis=0, concat_axis=0, tiled=True)
    returned, gate_grad, up_grad, down_grad, channel_sum, squares = lax.optimization_barrier(
        (returned, gate_grad, up_grad, down_grad, channel_sum, squares)
    )
    back_all = returned.reshape(experts * capacity, model_width)
    route_sum = lax.dot_general(
        chosen, back_all, (((0,), (0,)), ((), ())), preferred_element_type=jnp.float32
    )
    mid_grad = (cotangent.astype(jnp.float32) + route_sum).astype(jnp.bfloat16)
    average = channel_sum / model_width
    variance = squares / model_width - average * average
    inv_scale = lax.rsqrt(variance + NORM_EPS)[:, None]
    normed = (values - average[:, None]) * inv_scale
    scaled = normed * norm_gain
    activated = jax.nn.silu(scaled).astype(jnp.bfloat16)
    grad_tokens = gathered_rows(mid_grad, "tp")
    proj_grad, grad_tokens = reduced_products(grad_tokens, activated, "sp")
    act_grad = lax.dot_general(
        grad_tokens, out_weight, (((1,), (1,)), ((), ())), preferred_element_type=jnp.float32
    )
    scaled_grad = act_grad * silu_grad(scaled) * norm_gain
    grad_total, corr_total = lax.psum(
        (jnp.sum(scaled_grad, axis=1), jnp.sum(scaled_grad * normed, axis=1)), "tp"
    )
    grad_mean = (grad_total / model_width)[:, None]
    grad_corr = (corr_total / model_width)[:, None]
    conv_grad = (inv_scale * (scaled_grad - grad_mean - normed * grad_corr)).astype(jnp.bfloat16)
    halo_width = conv_taps.shape[0] // 2
    padded = extended(conv_grad, (("sp", 0),), halo_width)
    seq_rows = conv_grad.shape[0]
    accumulated = jnp.zeros(conv_grad.shape, jnp.float32)
    for offset in range(conv_taps.shape[0]):
        lead = 2 * halo_width - offset
        accumulated = accumulated + conv_taps[offset] * padded[lead : lead + seq_rows]
    input_grad = accumulated.astype(jnp.bfloat16)
    return (gate_grad, up_grad, down_grad, proj_grad, input_grad)


def solution(mesh):
    in_specs = (
        P(("sp", "tp"), None),
        P(("sp", "tp"), None),
        P(("sp", "tp"), None),
        P(("sp", "tp"), None),
        P("sp", "tp"),
        P(None, "tp"),
        P("tp"),
        P("tp", None),
        P("sp", None, "tp"),
        P("sp", None, "tp"),
        P("sp", "tp", None),
    )
    out_specs = (
        P("sp", None, "tp"),
        P("sp", None, "tp"),
        P("sp", "tp", None),
        P("sp", "tp"),
        P("sp", "tp"),
    )
    return jax.shard_map(
        per_device, mesh=mesh, in_specs=in_specs, out_specs=out_specs, check_vma=False
    )
```

```python
import jax
import jax.numpy as jnp
from jax import lax
from jax.sharding import PartitionSpec as P

NORM_EPS = 1e-05


def extended(block, sides, width):
    for axis, dim in sides:
        count = lax.axis_size(axis)
        forward = [(i, i + 1) for i in range(count - 1)]
        backward = [(target, source) for source, target in forward]
        low = lax.ppermute(
            lax.slice_in_dim(block, block.shape[dim] - width, None, axis=dim), axis, forward
        )
        high = lax.ppermute(lax.slice_in_dim(block, 0, width, axis=dim), axis, backward)
        block = jnp.concatenate([low, block, high], axis=dim)
    return block


def silu_grad(pre_act):
    logistic = jax.nn.sigmoid(pre_act)
    return logistic * (1.0 + pre_act * (1.0 - logistic))


def slot_targets(routes, experts, capacity):
    token_count, per_token = routes.shape
    flattened = routes.reshape(token_count * per_token)
    one_hot = flattened[:, None] == jnp.arange(experts, dtype=jnp.int32)[None, :]
    route_ids = jnp.arange(token_count * per_token, dtype=jnp.int32)
    before = (route_ids[None, :] < route_ids[:, None]).astype(jnp.bfloat16)
    earlier = jnp.dot(before, one_hot.astype(jnp.bfloat16), preferred_element_type=jnp.float32)
    positions = jnp.sum(jnp.where(one_hot, earlier, 0.0), axis=1).astype(jnp.int32)
    return (flattened * capacity + positions).reshape(token_count, per_token)


def halving_orders(count):
    bits = count.bit_length() - 1
    turned = min(bits, 3)
    return [
        [(start + step) % turned for step in range(turned)] + list(range(turned, bits))
        for start in range(turned)
    ]


def column_groups(columns, groups):
    lanes = 128
    tiles = columns // lanes
    sizes = [tiles // groups + (1 if g < tiles % groups else 0) for g in range(groups)]
    starts = [sum(sizes[:g]) * lanes for g in range(groups)]
    return [(start, size * lanes) for start, size in zip(starts, sizes) if size]


def picked(block, place, dim):
    return lax.dynamic_index_in_dim(block, place, dim, keepdims=False)


def reduced_products(rows, columns, axis):
    count = lax.axis_size(axis)
    tokens, width = rows.shape
    bits = count.bit_length() - 1
    own = lax.axis_index(axis)
    product = transposed_product(rows, columns).astype(jnp.bfloat16)
    cut = product.reshape((2,) * bits + (width // count, columns.shape[1]))
    orders = halving_orders(count)
    groups = column_groups(columns.shape[1], len(orders))
    orders = orders[: len(groups)]
    totals = [lax.slice_in_dim(cut, start, start + size, axis=bits + 1) for start, size in groups]
    left = [list(range(bits - 1, -1, -1)) for _ in groups]
    for step in range(bits):
        outgoing, kept = [], []
        for total, order, dims in zip(totals, orders, left):
            mine = (own >> order[step]) & 1
            dim = dims.index(order[step])
            dims.pop(dim)
            outgoing.append(picked(total, 1 - mine, dim).astype(jnp.bfloat16))
            kept.append(picked(total, mine, dim).astype(jnp.float32))
        if step == 0:
            outgoing, rows = lax.optimization_barrier((outgoing, rows))
        arrived = [
            lax.ppermute(block, axis, [(i, i ^ (1 << order[step])) for i in range(count)])
            for block, order in zip(outgoing, orders)
        ]
        arrived = lax.optimization_barrier(arrived)
        totals = [own_part + got.astype(jnp.float32) for own_part, got in zip(kept, arrived)]
    return jnp.concatenate(totals, axis=1), rows


def row_product(rows, matrix, dim=0):
    return lax.dot_general(
        rows, matrix, (((1,), (dim,)), ((), ())), preferred_element_type=jnp.float32
    )


def transposed_product(left, right):
    return lax.dot_general(
        left, right, (((0,), (0,)), ((), ())), preferred_element_type=jnp.float32
    )


def from_partner(block, axis):
    count = lax.axis_size(axis)
    return [
        lax.ppermute(block, axis, [(i, (i + step) % count) for i in range(count)])
        for step in range(1, count)
    ]


def hidden_gradients(pre_gate, pre_up, routed, down_mat):
    gate_act = jax.nn.silu(pre_gate)
    hidden = (gate_act * pre_up).astype(jnp.bfloat16)
    hidden_grad = row_product(routed, down_mat, 1)
    gate_pre = (hidden_grad * pre_up * silu_grad(pre_gate)).astype(jnp.bfloat16)
    up_pre = (hidden_grad * gate_act).astype(jnp.bfloat16)
    return hidden, gate_pre, up_pre


def input_part(gate_pre, up_pre, gate_mat, up_mat):
    return (row_product(gate_pre, gate_mat, 1) + row_product(up_pre, up_mat, 1)).astype(
        jnp.bfloat16
    )


def expert_backward(got_in, got_cot, gate_mat, up_mat, down_mat, axis):
    count = lax.axis_size(axis)
    all_in = [got_in] + from_partner(got_in, axis)
    pre = [(row_product(rows, gate_mat), row_product(rows, up_mat)) for rows in all_in]
    pre, got_cot = lax.optimization_barrier((pre, got_cot))
    all_cot = [got_cot] + from_partner(got_cot, axis)
    grads = [hidden_gradients(g, u, c, down_mat) for (g, u), c in zip(pre, all_cot)]
    back = None
    for step in range(1, count):
        part = input_part(grads[step][1], grads[step][2], gate_mat, up_mat)
        arrived = lax.ppermute(part, axis, [(i, (i - step) % count) for i in range(count)])
        back = (arrived,) if back is None else back + (arrived,)
    back_rows = input_part(grads[0][1], grads[0][2], gate_mat, up_mat).astype(jnp.float32)
    for arrived in back or ():
        back_rows = back_rows + arrived.astype(jnp.float32)
    gate_part = sum(transposed_product(x, g[1]) for x, g in zip(all_in, grads))
    up_part = sum(transposed_product(x, g[2]) for x, g in zip(all_in, grads))
    down_part = sum(transposed_product(g[0], c) for g, c in zip(grads, all_cot))
    return gate_part, up_part, down_part, back_rows.astype(jnp.bfloat16)


def gathered_rows(block, axis):
    count = lax.axis_size(axis)
    own = lax.axis_index(axis)
    blocks = [block] + from_partner(block, axis)
    turned = jnp.concatenate(blocks, axis=0)
    result = turned
    for place in range(1, count):
        order = [blocks[(place - i) % count] for i in range(count)]
        result = jnp.where(own == place, jnp.concatenate(order, axis=0), result)
    first = [blocks[-i % count] for i in range(count)]
    return jnp.where(own == 0, jnp.concatenate(first, axis=0), result)


def per_device(
    mid_rows,
    cotangent,
    routes,
    route_weight,
    filtered,
    conv_taps,
    norm_gain,
    out_weight,
    gate_weight,
    up_weight,
    down_weight,
):
    sp_count = lax.axis_size("sp")
    token_count, model_width = mid_rows.shape
    per_token = routes.shape[1]
    local_experts = gate_weight.shape[0]
    experts = local_experts * sp_count
    capacity = 2 * token_count * per_token // sp_count
    values = filtered.astype(jnp.float32)
    channel_sum, squares = lax.psum(
        (jnp.sum(values, axis=1), jnp.sum(values * values, axis=1)), "tp"
    )
    half = sp_count // 2
    side = lax.axis_index("sp") // half
    target = slot_targets(routes, experts, capacity)
    slot_ids = jnp.arange(experts * capacity, dtype=jnp.int32)
    chosen = jnp.any(slot_ids[:, None, None] == target[None, :, :], axis=2).astype(jnp.bfloat16)

    def with_far(block):
        far = lax.ppermute(block, "sp", [(i, (i + half) % sp_count) for i in range(sp_count)])
        return jnp.concatenate([block, far], axis=0)

    both_target, both_weight = with_far(target), with_far(route_weight)
    expert = both_target // capacity - side * half * local_experts
    origin = jnp.concatenate(
        [jnp.full((token_count, 1), side), jnp.full((token_count, 1), 1 - side)], axis=0
    )
    place = (expert // local_experts * 2 + origin) * local_experts + expert % local_experts
    place = place * capacity + both_target % capacity
    place = jnp.where((expert >= 0) & (expert < half * local_experts), place, -1)
    holds = slot_ids[:, None, None] == place[None, :, :]
    sent = jnp.any(holds, axis=2).astype(jnp.bfloat16)
    route_scale = jnp.sum(jnp.where(holds, both_weight[None, :, :], 0.0), axis=(1, 2))

    def within_half(block):
        return lax.all_to_all(
            block.reshape(half, 2, local_experts, capacity, model_width),
            "sp",
            split_axis=0,
            concat_axis=0,
            axis_index_groups=[[s * half + i for i in range(half)] for s in range(2)],
            tiled=True,
        )

    both_mid = with_far(mid_rows)
    both_mid, near_cot = lax.optimization_barrier((both_mid, cotangent))
    both_cot = with_far(near_cot)
    inputs = jnp.dot(sent, both_mid, preferred_element_type=jnp.float32).astype(jnp.bfloat16)
    got_in = within_half(inputs)
    cot_rows = jnp.dot(sent, both_cot, preferred_element_type=jnp.float32)
    routed = (route_scale[:, None] * cot_rows).astype(jnp.bfloat16)
    got_cot = within_half(routed)
    by_expert = (sp_count, local_experts, capacity, model_width)
    parts = [
        expert_backward(
            got_in[:, :, e].reshape(sp_count * capacity, model_width),
            got_cot[:, :, e].reshape(sp_count * capacity, model_width),
            gate_weight[e],
            up_weight[e],
            down_weight[e],
            "tp",
        )
        for e in range(local_experts)
    ]
    gate_grad, up_grad, down_grad = (
        jnp.stack([part[i] for part in parts], axis=0) for i in range(3)
    )
    back_rows = jnp.stack(
        [
            part[3].reshape(half, 2, capacity, model_width).transpose(1, 0, 2, 3)
            for part in parts
        ],
        axis=2,
    ).reshape(by_expert)
    returned = lax.all_to_all(back_rows, "sp", split_axis=0, concat_axis=0, tiled=True)
    returned, gate_grad, up_grad, down_grad, channel_sum, squares = lax.optimization_barrier(
        (returned, gate_grad, up_grad, down_grad, channel_sum, squares)
    )
    back_all = returned.reshape(experts * capacity, model_width)
    route_sum = lax.dot_general(
        chosen, back_all, (((0,), (0,)), ((), ())), preferred_element_type=jnp.float32
    )
    mid_grad = (cotangent.astype(jnp.float32) + route_sum).astype(jnp.bfloat16)
    average = channel_sum / model_width
    variance = squares / model_width - average * average
    inv_scale = lax.rsqrt(variance + NORM_EPS)[:, None]
    normed = (values - average[:, None]) * inv_scale
    scaled = normed * norm_gain
    activated = jax.nn.silu(scaled).astype(jnp.bfloat16)
    grad_tokens = gathered_rows(mid_grad, "tp")
    proj_grad, grad_tokens = reduced_products(grad_tokens, activated, "sp")
    act_grad = lax.dot_general(
        grad_tokens, out_weight, (((1,), (1,)), ((), ())), preferred_element_type=jnp.float32
    )
    scaled_grad = act_grad * silu_grad(scaled) * norm_gain
    grad_total, corr_total = lax.psum(
        (jnp.sum(scaled_grad, axis=1), jnp.sum(scaled_grad * normed, axis=1)), "tp"
    )
    grad_mean = (grad_total / model_width)[:, None]
    grad_corr = (corr_total / model_width)[:, None]
    conv_grad = (inv_scale * (scaled_grad - grad_mean - normed * grad_corr)).astype(jnp.bfloat16)
    halo_width = conv_taps.shape[0] // 2
    padded = extended(conv_grad, (("sp", 0),), halo_width)
    seq_rows = conv_grad.shape[0]
    accumulated = jnp.zeros(conv_grad.shape, jnp.float32)
    for offset in range(conv_taps.shape[0]):
        lead = 2 * halo_width - offset
        accumulated = accumulated + conv_taps[offset] * padded[lead : lead + seq_rows]
    input_grad = accumulated.astype(jnp.bfloat16)
    return (gate_grad, up_grad, down_grad, proj_grad, input_grad)


def solution(mesh):
    in_specs = (
        P(("sp", "tp"), None),
        P(("sp", "tp"), None),
        P(("sp", "tp"), None),
        P(("sp", "tp"), None),
        P("sp", "tp"),
        P(None, "tp"),
        P("tp"),
        P("tp", None),
        P("sp", None, "tp"),
        P("sp", None, "tp"),
        P("sp", "tp", None),
    )
    out_specs = (
        P("sp", None, "tp"),
        P("sp", None, "tp"),
        P("sp", "tp", None),
        P("sp", "tp"),
        P("sp", "tp"),
    )
    return jax.shard_map(
        per_device, mesh=mesh, in_specs=in_specs, out_specs=out_specs, check_vma=False
    )
```
